32 devices in a mesh: ep: 16 (over z, y, x), tp: 2 (over core).
Axes of the slice: x: 2, y: 2, z: 4, core: 2. Of those that a mesh axis runs over, the one named last changes fastest.
Arguments:
- tokens: bfloat16 [4096, 1024], P('ep'), may hold values from -6 to 6
- norm_gain: float32 [1024], replicated, may hold values from 0.1 to 1.9
- routing: int32 [4096, 2], P('ep'), may hold values from 0 to 31, all different within a row; in each aligned block of 256 rows (0 to 255, 256 to 511, ...) at most 16 rows name the same one
- route_weights: float32 [4096, 2], P('ep'), may hold values from 0.1 to 1
- lengths: int32 [1024], P('ep'), may hold values from 1 to 4, 2560 in all
- w_gate: bfloat16 [32, 1024, 3584], P('ep', None, 'tp'), may hold values from -0.1875 to 0.1875
- w_up: bfloat16 [32, 1024, 3584], P('ep', None, 'tp'), may hold values from -0.1875 to 0.1875
- w_down: bfloat16 [32, 3584, 1024], P('ep', 'tp'), may hold values from -0.09375 to 0.09375
Outputs:
- mixed: bfloat16 [4096, 1024], P('ep', 'tp')
The draws below stay inside these ranges and needn't reach their ends.
Inputs may be any that keep to these rules, and one draw needn't show every extreme that they name: `routing`: each row names 2 different experts; at most 16 rows of one device name the same expert, and that many is reached.
All inputs are finite; a program needn't handle non-finite values. No bound on the sum of `lengths` on one device may be relied on, other than what follows from the above.
Results may differ from the reference program's by a relative error of at most 0.009.
Values may be sent and summed in bfloat16 or wider, within the bound.
A program may use at most 64 MiB of HBM per device.

```python
import math
import jax
import jax.numpy as jnp
import numpy as np
from jax import lax

D = 1024
FFE = 3584
TOPK = 2
SPAN = 4
TOK_DEV = 256
EXPERTS = 32
CAP = 16
SEQS = 1024
TOKENS = 4096
N_TP = 2


def block_scale(rng, shape, shards, least, top_value):
    factor_of, own = 1.0, jax.random.fold_in(rng, 6)
    for dim, shards_of in shards:
        steps = jnp.exp(jax.random.uniform(jax.random.fold_in(own, dim), (shards_of,), jnp.float32, least / len(shards), top_value / len(shards)))
        factor_of = factor_of * jnp.repeat(steps, shape[dim] // shards_of).reshape([-1 if axis == dim else 1 for axis in range(len(shape))])
    return factor_of


def length_profile(count, total, reach, skew):
    loads = [(1 << 20) // math.isqrt(standing ** skew) + 1 for standing in range(2, count + 1)]
    spare, given = total - reach - (count - 1), [1] * (count - 1)
    while spare > 0:
        candidates = [i for i in range(count - 1) if given[i] < reach]
        whole, remaining = sum([loads[i] for i in candidates]), spare
        for i in candidates:
            more = min(reach - given[i], max(1, remaining * loads[i] // whole), spare)
            given[i] = given[i] + more
            spare = spare - more
    return np.array([reach] + given)


def uneven_parts(stream_key, count, total, most, slope):
    if count == 2:
        one = jax.random.randint(stream_key, (), max(1, total - most), min(most, total - 1) + 1)
        return jnp.stack([one, total - one])
    sizes = jnp.asarray(length_profile(count, total, most, slope), jnp.int32)
    twos = (count - 1) // 2
    giver, receiver = sizes[1:1 + 2 * twos:2], sizes[2:2 + 2 * twos:2]
    room = jnp.minimum(giver - 1, most - receiver)
    passed = jax.random.randint(jax.random.fold_in(stream_key, 1), (twos,), 0, 1 << 20) % (room + 1)
    sizes = sizes.at[1:1 + 2 * twos:2].set(giver - passed).at[2:2 + 2 * twos:2].set(receiver + passed)
    return sizes[jax.random.permutation(jax.random.fold_in(stream_key, 2), count)]


def assign_block(stream_key, own, number, rows, count, top, reach, lean):
    order = jax.random.permutation(stream_key, count)
    heavy_load, ordinary = shares(count, rows * top, reach, lean, True), shares(count, rows * top, reach, lean, False)
    places = jnp.arange(count)

    def named(sizes, rotation):
        used = int((sizes > 0).sum())
        fixed = max(1, used // 4)
        shifted = fixed + (places - fixed + rotation * (used - fixed)) % max(1, count - fixed)
        return jnp.zeros((count,), jnp.int32).at[order[jnp.where(places < fixed, places, shifted)]].set(jnp.asarray(sizes, jnp.int32))

    sizes = jnp.where(number % 4 == 0, named(heavy_load, number // 4), named(ordinary, number - number // 4 - 1))
    mixed = jax.random.permutation(jax.random.fold_in(own, 3), count)
    source_of, sink = mixed[0:count // 2 * 2:2], mixed[1:count // 2 * 2:2]
    margin = jnp.minimum(sizes[source_of] - 1, reach - sizes[sink]) // 2
    margin = jnp.where((source_of == order[0]) | (sink == order[0]) | (sizes[sink] == 0), 0, jnp.maximum(margin, 0))
    shifted = jax.random.randint(jax.random.fold_in(own, 4), (count // 2,), 0, 1 << 20) % (margin + 1)
    sizes = sizes.at[source_of].add(-shifted).at[sink].add(shifted)
    members = jnp.searchsorted(jnp.cumsum(sizes), jnp.arange(rows * top), side="right").astype(jnp.int32)
    table = members.reshape(top, rows).T
    table = table[jax.random.permutation(jax.random.fold_in(own, 1), rows)]
    rotation = jax.random.randint(jax.random.fold_in(own, 2), (rows, 1), 0, top)
    return jnp.take_along_axis(table, (jnp.arange(top)[None, :] + rotation) % top, axis=1)


def shares(count, total, reach, slope, full):
    weights = [(1 << 20) // math.isqrt(grade ** slope) + 1 for grade in range(1, count + 1)]
    largest = reach if full else min(reach, max(-(-total // count), total * weights[0] // sum(weights)))
    least = 1 if total - largest >= count - 1 else 0
    holding, spare = [largest] + [least] * (count - 1), total - largest - least * (count - 1)
    while spare > 0:
        movable = [i for i in range(1, count) if holding[i] < largest] or [i for i in range(1, count) if holding[i] < reach]
        whole, remaining = sum([weights[i] for i in movable]), spare
        for i in movable:
            addition = min(reach - holding[i], max(1, remaining * weights[i] // whole), spare)
            holding[i] = holding[i] + addition
            spare = spare - addition
    return np.array(holding)


def bell_draw(rng, shape, deviation, most, split=(), kind=jnp.bfloat16):
    array = deviation * jax.random.normal(rng, shape, jnp.float32)
    if split:
        array = array * block_scale(rng, shape, split, -0.22, 0.18)
    return jnp.clip(array, -most, most).astype(kind)


def setup_inputs(seed: int = 0) -> dict:
    key_list = jax.random.split(jax.random.key(seed), 9)
    tokens = bell_draw(key_list[0], (TOKENS, D), 1.0, 6.0, ((0, 16),))
    norm_gain = jnp.clip(1.0 + 0.18 * jax.random.normal(key_list[1], (D,), jnp.float32), 0.1, 1.9)
    routing_keys = jax.random.split(jax.random.fold_in(key_list[2], 1), TOKENS // TOK_DEV)
    routing_turns = jax.random.permutation(jax.random.fold_in(key_list[2], 3), TOKENS // TOK_DEV)
    routing = jax.vmap(lambda own, number: assign_block(jax.random.fold_in(key_list[2], 2), own, number, TOK_DEV, EXPERTS, TOPK, CAP, 2))(routing_keys, routing_turns).reshape((TOKENS, TOPK))
    route_weights = jnp.clip(0.1 + 0.9 * jax.random.uniform(key_list[3], (TOKENS, TOPK), jnp.float32) ** block_scale(key_list[3], (TOKENS, TOPK), ((0, 16),), -0.2, 0.2), 0.1, 1.0)
    lengths = uneven_parts(key_list[4], SEQS, SEQS * 5 // 2, SPAN, 2).astype(jnp.int32)
    w_gate = bell_draw(key_list[5], (EXPERTS, D, FFE), D ** -0.5, 0.1875, ((0, 16), (2, 2)))
    w_up = bell_draw(key_list[6], (EXPERTS, D, FFE), D ** -0.5, 0.1875, ((0, 16), (2, 2)))
    w_down = bell_draw(key_list[7], (EXPERTS, FFE, D), FFE ** -0.5, 0.09375, ((0, 16), (1, 2)))
    return {"tokens": tokens, "norm_gain": norm_gain, "routing": routing, "route_weights": route_weights, "lengths": lengths, "w_gate": w_gate, "w_up": w_up, "w_down": w_down}


eps = 1e-06
block_rows = 64

def expert_rows(row_block, gate_mat, up_mat, down_mat):
    gate_proj = jnp.dot(row_block, gate_mat, preferred_element_type=jnp.float32)
    up_proj = jnp.dot(row_block, up_mat, preferred_element_type=jnp.float32)
    hidden = (jax.nn.silu(gate_proj) * up_proj).astype(jnp.bfloat16)
    half_width = FFE // N_TP
    summed = jnp.zeros((row_block.shape[0], D), jnp.float32)
    for core_part in range(N_TP):
        partial_value = jnp.dot(hidden[:, core_part * half_width:(core_part + 1) * half_width], down_mat[core_part * half_width:(core_part + 1) * half_width], preferred_element_type=jnp.float32)
        rounded = lax.optimization_barrier(partial_value.astype(jnp.bfloat16))
        summed = summed + rounded.astype(jnp.float32)
    return summed.astype(jnp.bfloat16)

def reference(tokens, norm_gain, routing, route_weights, lengths, w_gate, w_up, w_down):
    floats = tokens.astype(jnp.float32)
    normed = (floats * lax.rsqrt(lax.optimization_barrier(jnp.mean(floats * floats, axis=-1, keepdims=True)) + eps) * norm_gain).astype(jnp.bfloat16)
    position = jnp.arange(TOKENS, dtype=jnp.int32)
    live_rows = position % SPAN < lengths[position // SPAN]
    flat_ids = jnp.where(live_rows[:, None], routing, EXPERTS).reshape(-1).astype(jnp.int32)
    sorted_picks = jnp.argsort(flat_ids, stable=True).astype(jnp.int32)
    owner_rows = (sorted_picks // TOPK).astype(jnp.int32)
    weight_of = route_weights.reshape(-1)[sorted_picks]
    counts = lax.optimization_barrier(jnp.sum((flat_ids[:, None] == jnp.arange(EXPERTS, dtype=jnp.int32)[None, :]).astype(jnp.int32), axis=0))
    starts = (jnp.cumsum(counts) - counts).astype(jnp.int32)
    total_picks = TOKENS * TOPK

    def expert_step(expert, totals):
        gate_mat = w_gate[expert]
        up_mat = w_up[expert]
        down_mat = w_down[expert]
        first = starts[expert]
        amount = counts[expert]

        def has_more(carry_state):
            return carry_state[0] * block_rows < amount

        def block_step(carry_state):
            block_no, inner = carry_state
            pick_index = first + block_no * block_rows + jnp.arange(block_rows, dtype=jnp.int32)
            in_range = pick_index < first + amount
            clipped = jnp.minimum(pick_index, total_picks - 1).astype(jnp.int32)
            rows_at = owner_rows[clipped]
            result = expert_rows(normed[rows_at], gate_mat, up_mat, down_mat)
            factor = jnp.where(in_range, weight_of[clipped], 0.0)
            inner = inner.at[rows_at].add(factor[:, None] * result.astype(jnp.float32))
            return (block_no + 1, inner)
        ended = lax.while_loop(has_more, block_step, (jnp.int32(0), totals))
        return ended[1]
    totals = lax.fori_loop(0, EXPERTS, expert_step, jnp.zeros((TOKENS, D), jnp.float32))
    return totals.astype(jnp.bfloat16)
```

```python
import functools

import jax
import jax.numpy as jnp
from jax import lax
from jax.experimental import pallas as pl
from jax.experimental.pallas import tpu as pltpu
from jax.sharding import PartitionSpec as P

MESH = pl.DeviceIdType.MESH
GROUPS = 2
TILE = 16
eps = 1e-06
BF = jnp.bfloat16
F32 = jnp.float32


def dot(a, b):
    return jnp.dot(a, b, preferred_element_type=F32)


def kernel(
    n, groups, local, bound, span,
    gain_ref, routing_ref, weights_ref, lengths_ref,
    tokens_hbm, gate_hbm, up_hbm, down_hbm,
    out_ref,
    tok, gate_w, up_w, down_w, outgoing, incoming, hidden, partial, theirs, returning, returned, comb,
    tok_sem, w_sem, disp_send, disp_recv, fwd_send, fwd_recv, part_send, part_recv, ret_send, ret_recv,
):
    me = lax.axis_index("ep")
    core = lax.axis_index("tp")
    other = 1 - core
    pow2 = n & (n - 1) == 0
    per = n // groups
    rows = per * bound
    group_slots = local * rows
    tok_rows, width = tok.shape
    half = width // 2
    chosen = routing_ref.shape[0]
    experts = n * local
    mine = pl.ds(pl.multiple_of(core * half, half), half)

    def target(k):
        return lax.bitwise_xor(me, k) if pow2 else lax.rem(me + k, n)

    barrier = pltpu.get_barrier_semaphore()
    for k in range(1, n):
        pl.semaphore_signal(barrier, inc=1, device_id=(target(k), core), device_id_type=MESH)
    pl.semaphore_signal(barrier, inc=1, device_id=(me, other), device_id_type=MESH)

    tok_copy = pltpu.make_async_copy(tokens_hbm, tok, tok_sem)
    tok_copy.start()
    loads = {}
    for x in range(local):
        for i, (src, dst) in enumerate(((gate_hbm, gate_w), (up_hbm, up_w), (down_hbm, down_w))):
            loads[x, i] = pltpu.make_async_copy(src.at[x], dst.at[x], w_sem.at[x, i])
            loads[x, i].start()

    count = lengths_ref.shape[1]
    spread = (
        lax.broadcasted_iota(jnp.int32, (count, tok_rows), 1) // span
        == lax.broadcasted_iota(jnp.int32, (count, tok_rows), 0)
    ).astype(BF)
    lens = jnp.broadcast_to(lengths_ref[...].astype(F32), (8, count)).astype(BF)
    live_len = dot(lens, spread)[0:1]
    place = lax.broadcasted_iota(jnp.int32, (1, tok_rows), 1) % span
    live = place.astype(F32) < live_len
    routing = routing_ref[...]
    ids = lax.broadcasted_iota(jnp.int32, (experts, tok_rows), 0)
    named = ids == routing[0:1]
    for i in range(1, chosen):
        named = named | (ids == routing[i : i + 1])
    named = named & live
    earlier = (
        lax.broadcasted_iota(jnp.int32, (tok_rows, tok_rows), 0)
        < lax.broadcasted_iota(jnp.int32, (tok_rows, tok_rows), 1)
    ).astype(BF)
    rank = dot(jnp.where(named, 1.0, 0.0).astype(BF), earlier)
    rank = jnp.where(named, rank, -1.0).astype(BF)

    def slot_ids(shape, g):
        s = lax.broadcasted_iota(jnp.int32, shape, 0)
        k = (s // bound) % per * groups + g
        peer = lax.bitwise_xor(jnp.full(shape, me, jnp.int32), k) if pow2 else (me + k) % n
        return peer * local + s // rows, s % bound

    tok_copy.wait()
    floats = tok[...].astype(F32)
    scale = lax.rsqrt(jnp.mean(floats * floats, axis=-1, keepdims=True) + eps)
    normed = (tok[:, mine].astype(F32) * scale * gain_ref[:, mine]).astype(BF)

    def dispatch(k):
        g, j = k % groups, k // groups
        return pltpu.make_async_remote_copy(
            src_ref=outgoing.at[g, :, j],
            dst_ref=incoming.at[g, :, j, :, mine],
            send_sem=disp_send.at[k],
            recv_sem=disp_recv.at[k],
            device_id=(target(k), core),
            device_id_type=MESH,
        )

    def forward(k):
        g, j = k % groups, k // groups
        return pltpu.make_async_remote_copy(
            src_ref=incoming.at[g, :, j, :, mine],
            dst_ref=incoming.at[g, :, j, :, mine],
            send_sem=fwd_send.at[k],
            recv_sem=fwd_recv.at[k],
            device_id=(me, other),
            device_id_type=MESH,
        )

    def swap(g, x):
        return pltpu.make_async_remote_copy(
            src_ref=partial.at[g, x, other],
            dst_ref=theirs.at[g, x],
            send_sem=part_send.at[g, x],
            recv_sem=part_recv.at[g, x],
            device_id=(me, other),
            device_id_type=MESH,
        )

    def give_back(k, x):
        g, j = k % groups, k // groups
        return pltpu.make_async_remote_copy(
            src_ref=returning.at[g, x, j],
            dst_ref=returned.at[g, x, j],
            send_sem=ret_send.at[k, x],
            recv_sem=ret_recv.at[k, x],
            device_id=(target((n - k) % n if not pow2 else k), core),
            device_id_type=MESH,
        )

    def members(g):
        return list(range(g, n, groups))

    for g in range(groups):
        owner, slot = slot_ids((group_slots, experts), g)
        to_expert = (owner == lax.broadcasted_iota(jnp.int32, (group_slots, experts), 1)).astype(BF)
        owner, slot = slot_ids((group_slots, tok_rows), g)
        hit = dot(to_expert, rank) == slot.astype(F32)
        block = dot(jnp.where(hit, 1.0, 0.0).astype(BF), normed).astype(BF)
        block = block.reshape(local, per, bound, half)
        outgoing[g] = block
        if g == 0:
            incoming[0, :, 0, :, mine] = block[:, 0]
            pl.semaphore_wait(barrier, n)
        for k in reversed(members(g)):
            if k:
                dispatch(k).start()
        if g == 0:
            forward(0).start()
    for g in range(groups):
        owner, slot = slot_ids((group_slots, experts), g)
        to_expert = (owner == lax.broadcasted_iota(jnp.int32, (group_slots, experts), 1)).astype(BF)
        owner, slot = slot_ids((group_slots, tok_rows), g)
        hit = dot(to_expert, rank) == slot.astype(F32)
        value = jnp.zeros((group_slots, tok_rows), F32)
        for i in range(chosen):
            value = jnp.where(owner == routing[i : i + 1], weights_ref[i : i + 1], value)
        comb[g] = jnp.where(hit, value, 0.0).T

    def arrive(g):
        for k in members(g):
            if k:
                dispatch(k).wait_recv()
                forward(k).start()

    arrive(0)
    for g in range(groups):
        for k in members(g):
            forward(k).wait_recv()
        for x in range(local):
            xs = incoming[g, x].reshape(rows, width)
            if g == 0:
                loads[x, 0].wait()
            gate = dot(xs, gate_w[x])
            if g == 0:
                loads[x, 1].wait()
            hidden[...] = (gate / (1.0 + jnp.exp(-gate)) * dot(xs, up_w[x])).astype(BF)
            if g == 0:
                loads[x, 2].wait()
            down = dot(hidden[...], down_w[x]).astype(BF)
            partial[g, x, 0] = down[:, :half]
            partial[g, x, 1] = down[:, half:]
            swap(g, x).start()
        if g + 1 < groups:
            arrive(g + 1)
        for x in range(local):
            swap(g, x).wait_recv()
            total = (partial[g, x, core].astype(F32) + theirs[g, x].astype(F32)).astype(BF)
            total = total.reshape(per, bound, half)
            returning[g, x] = total
            if g == 0:
                returned[0, x, 0] = total[0]
            for k in reversed(members(g)):
                if k:
                    give_back(k, x).start()
    mixed = jnp.zeros((tok_rows, half), F32)
    for g in range(groups):
        for x in range(local):
            for k in members(g):
                if k:
                    give_back(k, x).wait_recv()
        values = returned[g].reshape(group_slots, half)
        weight = comb[g]
        high = weight.astype(BF)
        low = (weight - high.astype(F32)).astype(BF)
        mixed = mixed + dot(high, values) + dot(low, values)
    out_ref[...] = mixed.astype(BF)
    for k in range(n):
        if k:
            dispatch(k).wait_send()
            for x in range(local):
                give_back(k, x).wait_send()
        forward(k).wait_send()
    for g in range(groups):
        for x in range(local):
            swap(g, x).wait_send()


def per_device(n, tokens, norm_gain, routing, route_weights, lengths, w_gate, w_up, w_down):
    local, width, units = w_gate.shape
    tok_rows, chosen = routing.shape
    experts = n * local
    groups = GROUPS
    bound = 2 * ((tok_rows * chosen + 2 * experts - 1) // (2 * experts))
    bound = (bound + TILE - 1) // TILE * TILE
    half = width // 2
    per = n // groups
    rows = per * bound
    span = tok_rows // lengths.shape[0]
    vmem = pl.BlockSpec(memory_space=pltpu.VMEM)
    hbm = pl.BlockSpec(memory_space=pl.ANY)
    dma = pltpu.SemaphoreType.DMA
    return pl.pallas_call(
        functools.partial(kernel, n, groups, local, bound, span),
        out_shape=jax.ShapeDtypeStruct((tok_rows, half), BF),
        in_specs=[vmem] * 4 + [hbm] * 4,
        out_specs=vmem,
        scratch_shapes=[
            pltpu.VMEM((tok_rows, width), BF),
            pltpu.VMEM((local, width, units), BF),
            pltpu.VMEM((local, width, units), BF),
            pltpu.VMEM((local, units, width), BF),
            pltpu.VMEM((groups, local, per, bound, half), BF),
            pltpu.VMEM((groups, local, per, bound, width), BF),
            pltpu.VMEM((rows, units), BF),
            pltpu.VMEM((groups, local, 2, rows, half), BF),
            pltpu.VMEM((groups, local, rows, half), BF),
            pltpu.VMEM((groups, local, per, bound, half), BF),
            pltpu.VMEM((groups, local, per, bound, half), BF),
            pltpu.VMEM((groups, tok_rows, local * rows), F32),
            dma,
            dma((local, 3)),
            dma((n,)),
            dma((n,)),
            dma((n,)),
            dma((n,)),
            dma((groups, local)),
            dma((groups, local)),
            dma((n, local)),
            dma((n, local)),
        ],
        compiler_params=pltpu.CompilerParams(
            collective_id=0, has_side_effects=True, vmem_limit_bytes=63 * 1024 * 1024
        ),
    )(
        norm_gain.reshape(1, width),
        routing.T,
        route_weights.T,
        lengths.reshape(1, -1),
        tokens,
        w_gate,
        w_up,
        w_down,
    )


def solution(mesh):
    placed = (
        P("ep", None),
        P(),
        P("ep", None),
        P("ep", None),
        P("ep"),
        P("ep", None, "tp"),
        P("ep", None, "tp"),
        P("ep", "tp", None),
    )
    return jax.shard_map(
        functools.partial(per_device, mesh.shape["ep"]),
        mesh=mesh, in_specs=placed, out_specs=P("ep", "tp"), check_vma=False,
    )
```

```python
import functools

import jax
import jax.numpy as jnp
from jax import lax
from jax.experimental import pallas as pl
from jax.experimental.pallas import tpu as pltpu
from jax.sharding import PartitionSpec as P

MESH = pl.DeviceIdType.MESH
GROUPS = 2
TILE = 16
eps = 1e-06
BF = jnp.bfloat16
F32 = jnp.float32


def dot(a, b):
    return jnp.dot(a, b, preferred_element_type=F32)


def kernel(
    n, groups, local, bound, span,
    gain_hbm, routing_hbm, weights_hbm, lengths_hbm,
    tokens_hbm, gate_hbm, up_hbm, down_hbm,
    out_ref,
    gain_ref, routing_ref, weights_ref, lengths_ref, tok, gate_w, up_w, down_w, outgoing, incoming, hidden, partial, theirs, returning, returned, comb,
    small_sem, tok_sem, w_sem, disp_send, disp_recv, fwd_send, fwd_recv, part_send, part_recv, ret_send, ret_recv,
):
    me = lax.axis_index("ep")
    core = lax.axis_index("tp")
    other = 1 - core
    pow2 = n & (n - 1) == 0
    per = n // groups
    rows = per * bound
    group_slots = local * rows
    tok_rows, width = tok.shape
    half = width // 2
    chosen = routing_ref.shape[0]
    experts = n * local
    mine = pl.ds(pl.multiple_of(core * half, half), half)

    def target(k):
        return lax.bitwise_xor(me, k) if pow2 else lax.rem(me + k, n)

    small = [
        pltpu.make_async_copy(src, dst, small_sem.at[i])
        for i, (src, dst) in enumerate((
            (lengths_hbm, lengths_ref),
            (routing_hbm, routing_ref),
            (gain_hbm, gain_ref),
            (weights_hbm, weights_ref),
        ))
    ]
    tok_copy = pltpu.make_async_copy(tokens_hbm, tok, tok_sem)
    tok_copy.start()
    for copy in small:
        copy.start()

    barrier = pltpu.get_barrier_semaphore()
    for k in range(1, n):
        pl.semaphore_signal(barrier, inc=1, device_id=(target(k), core), device_id_type=MESH)
    pl.semaphore_signal(barrier, inc=1, device_id=(me, other), device_id_type=MESH)

    loads = {}
    for x in range(local):
        for i, (src, dst) in enumerate(((gate_hbm, gate_w), (up_hbm, up_w), (down_hbm, down_w))):
            loads[x, i] = pltpu.make_async_copy(src.at[x], dst.at[x], w_sem.at[x, i])
            loads[x, i].start()

    for copy in small:
        copy.wait()

    count = lengths_ref.shape[1]
    spread = (
        lax.broadcasted_iota(jnp.int32, (count, tok_rows), 1) // span
        == lax.broadcasted_iota(jnp.int32, (count, tok_rows), 0)
    ).astype(BF)
    lens = jnp.broadcast_to(lengths_ref[...].astype(F32), (8, count)).astype(BF)
    live_len = dot(lens, spread)[0:1]
    place = lax.broadcasted_iota(jnp.int32, (1, tok_rows), 1) % span
    live = place.astype(F32) < live_len
    routing = routing_ref[...]
    ids = lax.broadcasted_iota(jnp.int32, (experts, tok_rows), 0)
    named = ids == routing[0:1]
    for i in range(1, chosen):
        named = named | (ids == routing[i : i + 1])
    named = named & live
    earlier = (
        lax.broadcasted_iota(jnp.int32, (tok_rows, tok_rows), 0)
        < lax.broadcasted_iota(jnp.int32, (tok_rows, tok_rows), 1)
    ).astype(BF)
    rank = dot(jnp.where(named, 1.0, 0.0).astype(BF), earlier)
    rank = jnp.where(named, rank, -1.0).astype(BF)

    def slot_ids(shape, g):
        s = lax.broadcasted_iota(jnp.int32, shape, 0)
        k = (s // bound) % per * groups + g
        peer = lax.bitwise_xor(jnp.full(shape, me, jnp.int32), k) if pow2 else (me + k) % n
        return peer * local + s // rows, s % bound

    tok_copy.wait()
    floats = tok[...].astype(F32)
    scale = lax.rsqrt(jnp.mean(floats * floats, axis=-1, keepdims=True) + eps)
    normed = (tok[:, mine].astype(F32) * scale * gain_ref[:, mine]).astype(BF)

    def dispatch(k):
        g, j = k % groups, k // groups
        return pltpu.make_async_remote_copy(
            src_ref=outgoing.at[g, :, j],
            dst_ref=incoming.at[g, :, j, :, mine],
            send_sem=disp_send.at[k],
            recv_sem=disp_recv.at[k],
            device_id=(target(k), core),
            device_id_type=MESH,
        )

    def forward(k):
        g, j = k % groups, k // groups
        return pltpu.make_async_remote_copy(
            src_ref=incoming.at[g, :, j, :, mine],
            dst_ref=incoming.at[g, :, j, :, mine],
            send_sem=fwd_send.at[k],
            recv_sem=fwd_recv.at[k],
            device_id=(me, other),
            device_id_type=MESH,
        )

    def swap(g, x):
        return pltpu.make_async_remote_copy(
            src_ref=partial.at[g, x, other],
            dst_ref=theirs.at[g, x],
            send_sem=part_send.at[g, x],
            recv_sem=part_recv.at[g, x],
            device_id=(me, other),
            device_id_type=MESH,
        )

    def give_back(k, x):
        g, j = k % groups, k // groups
        return pltpu.make_async_remote_copy(
            src_ref=returning.at[g, x, j],
            dst_ref=returned.at[g, x, j],
            send_sem=ret_send.at[k, x],
            recv_sem=ret_recv.at[k, x],
            device_id=(target((n - k) % n if not pow2 else k), core),
            device_id_type=MESH,
        )

    def members(g):
        return list(range(g, n, groups))

    def fill(g):
        owner, slot = slot_ids((group_slots, experts), g)
        to_expert = (owner == lax.broadcasted_iota(jnp.int32, (group_slots, experts), 1)).astype(BF)
        owner, slot = slot_ids((group_slots, tok_rows), g)
        hit = dot(to_expert, rank) == slot.astype(F32)
        block = dot(jnp.where(hit, 1.0, 0.0).astype(BF), normed).astype(BF)
        block = block.reshape(local, per, bound, half)
        outgoing[g] = block
        if g == 0:
            incoming[0, :, 0, :, mine] = block[:, 0]

    def send(g):
        for k in reversed(members(g)):
            if k:
                dispatch(k).start()

    fill(0)
    pl.semaphore_wait(barrier, n)
    send(0)
    forward(0).start()
    for g in range(1, groups):
        fill(g)
        send(g)
    for g in range(groups):
        owner, slot = slot_ids((group_slots, experts), g)
        to_expert = (owner == lax.broadcasted_iota(jnp.int32, (group_slots, experts), 1)).astype(BF)
        owner, slot = slot_ids((group_slots, tok_rows), g)
        hit = dot(to_expert, rank) == slot.astype(F32)
        value = jnp.zeros((group_slots, tok_rows), F32)
        for i in range(chosen):
            value = jnp.where(owner == routing[i : i + 1], weights_ref[i : i + 1], value)
        comb[g] = jnp.where(hit, value, 0.0).T

    def arrive(g):
        for k in members(g):
            if k:
                dispatch(k).wait_recv()
                forward(k).start()

    def finish(g, x):
        swap(g, x).wait_recv()
        total = (partial[g, x, core].astype(F32) + theirs[g, x].astype(F32)).astype(BF)
        total = total.reshape(per, bound, half)
        returning[g, x] = total
        if g == 0:
            returned[0, x, 0] = total[0]
        for k in reversed(members(g)):
            if k:
                give_back(k, x).start()

    arrive(0)
    for g in range(groups):
        for k in members(g):
            forward(k).wait_recv()
        for x in range(local):
            xs = incoming[g, x].reshape(rows, width)
            if g == 0:
                loads[x, 0].wait()
            gate = dot(xs, gate_w[x])
            if g == 0:
                loads[x, 1].wait()
            hidden[...] = (gate / (1.0 + jnp.exp(-gate)) * dot(xs, up_w[x])).astype(BF)
            if g == 0:
                loads[x, 2].wait()
            if x:
                finish(g, x - 1)
            down = dot(hidden[...], down_w[x]).astype(BF)
            partial[g, x, 0] = down[:, :half]
            partial[g, x, 1] = down[:, half:]
            swap(g, x).start()
        if g + 1 < groups:
            arrive(g + 1)
        finish(g, local - 1)
    mixed = jnp.zeros((tok_rows, half), F32)
    for g in range(groups):
        for x in range(local):
            for k in members(g):
                if k:
                    give_back(k, x).wait_recv()
        values = returned[g].reshape(group_slots, half)
        weight = comb[g]
        high = weight.astype(BF)
        low = (weight - high.astype(F32)).astype(BF)
        mixed = mixed + dot(high, values) + dot(low, values)
    out_ref[...] = mixed.astype(BF)
    for k in range(n):
        if k:
            dispatch(k).wait_send()
            for x in range(local):
                give_back(k, x).wait_send()
        forward(k).wait_send()
    for g in range(groups):
        for x in range(local):
            swap(g, x).wait_send()


def per_device(n, tokens, norm_gain, routing, route_weights, lengths, w_gate, w_up, w_down):
    local, width, units = w_gate.shape
    tok_rows, chosen = routing.shape
    experts = n * local
    groups = GROUPS
    bound = 2 * ((tok_rows * chosen + 2 * experts - 1) // (2 * experts))
    bound = (bound + TILE - 1) // TILE * TILE
    half = width // 2
    per = n // groups
    rows = per * bound
    span = tok_rows // lengths.shape[0]
    vmem = pl.BlockSpec(memory_space=pltpu.VMEM)
    hbm = pl.BlockSpec(memory_space=pltpu.HBM)
    dma = pltpu.SemaphoreType.DMA
    return pl.pallas_call(
        functools.partial(kernel, n, groups, local, bound, span),
        out_shape=pltpu.VMEM((tok_rows, half), BF),
        in_specs=[hbm] * 8,
        out_specs=vmem,
        scratch_shapes=[
            pltpu.VMEM((1, width), F32),
            pltpu.VMEM((chosen, tok_rows), jnp.int32),
            pltpu.VMEM((chosen, tok_rows), F32),
            pltpu.VMEM((1, lengths.shape[0]), jnp.int32),
            pltpu.VMEM((tok_rows, width), BF),
            pltpu.VMEM((local, width, units), BF),
            pltpu.VMEM((local, width, units), BF),
            pltpu.VMEM((local, units, width), BF),
            pltpu.VMEM((groups, local, per, bound, half), BF),
            pltpu.VMEM((groups, local, per, bound, width), BF),
            pltpu.VMEM((rows, units), BF),
            pltpu.VMEM((groups, local, 2, rows, half), BF),
            pltpu.VMEM((groups, local, rows, half), BF),
            pltpu.VMEM((groups, local, per, bound, half), BF),
            pltpu.VMEM((groups, local, per, bound, half), BF),
            pltpu.VMEM((groups, tok_rows, local * rows), F32),
            dma((4,)),
            dma,
            dma((local, 3)),
            dma((n,)),
            dma((n,)),
            dma((n,)),
            dma((n,)),
            dma((groups, local)),
            dma((groups, local)),
            dma((n, local)),
            dma((n, local)),
        ],
        compiler_params=pltpu.CompilerParams(
            collective_id=0, has_side_effects=True, vmem_limit_bytes=66000000
        ),
    )(
        norm_gain.reshape(1, width),
        routing.T,
        route_weights.T,
        lengths.reshape(1, -1),
        tokens,
        w_gate,
        w_up,
        w_down,
    )


def solution(mesh):
    placed = (
        P("ep", None),
        P(),
        P("ep", None),
        P("ep", None),
        P("ep"),
        P("ep", None, "tp"),
        P("ep", None, "tp"),
        P("ep", "tp", None),
    )
    return jax.shard_map(
        functools.partial(per_device, mesh.shape["ep"]),
        mesh=mesh, in_specs=placed, out_specs=P("ep", "tp"), check_vma=False,
    )
```
